256 devices in a mesh: sp: 32 (over z, y), dp: 8 (over x, core).
Axes of the slice: x: 4, y: 4, z: 8, core: 2. Of those that a mesh axis runs over, the one named last changes fastest.
Arguments:
- hidden_states: bfloat16 [16, 4096, 2048], P('dp', 'sp'), may hold values from -288 to 288
- cumulative_gate: float32 [16, 4096, 32], P('dp', 'sp'), may hold values from -16384 to 0, as said below
- query_weight: bfloat16 [2048, 2048], P('dp'), may hold values from -0.125 to 0.125
- key_weight: bfloat16 [2048, 512], P('dp'), may hold values from -0.125 to 0.125
- value_weight: bfloat16 [2048, 512], P('dp'), may hold values from -0.125 to 0.125
- out_weight: bfloat16 [2048, 2048], P('dp'), may hold values from -0.75 to 0.75
Outputs:
- mixed: bfloat16 [16, 4096, 2048], P('dp', 'sp')
The draws below stay inside these ranges and needn't reach their ends.
Inputs may be any that keep to these rules, and one draw needn't show every extreme that they name: cumulative_gate never rises along a sequence and is at most 0.
All inputs are finite; a program needn't handle non-finite values.
Results may differ from the reference program's by a relative error of at most 0.009.
The reference program's roundings to bfloat16 on the way (of `query`, `key`, `value`, `weights` and `attended`) count: a program that leaves them out, or rounds other values in their place, can miss the bound.
Values may be sent and summed in bfloat16 or wider, within the bound.
No kernel may reach another device: no remote copies, remote signals or barrier semaphores. Data moves between devices by JAX's collectives and lax.ppermute only.
A program may use at most 64 MiB of HBM per device.

```python
import math
import jax
import jax.numpy as jnp
from jax import lax

D = 2048
HEADS = 32
KV_HEADS = 8
HEAD = 64
POS_DEV = 128
QW = 2048
KVW = 512
SEQUENCE_LENGTH = 4096
SEQS = 16


def draw_hidden_states(key, part):
    random_keys = jax.random.split(jax.random.fold_in(key, 3), 1)
    values = jnp.clip(jax.random.normal(random_keys[0], (SEQS, SEQUENCE_LENGTH, D), jnp.float32), -6.0, 6.0)
    return values.astype(jnp.bfloat16)


def draw_cumulative_gate(key, part):
    random_keys = jax.random.split(jax.random.fold_in(key, 7), 7)
    order = jax.random.permutation(random_keys[0], HEADS)
    sluggish_heads = order < HEADS // 2
    slow_rate = 0.5
    tensor_extent = (SEQS, SEQUENCE_LENGTH, HEADS)
    jaggedness = jax.random.uniform(random_keys[1], tensor_extent, jnp.float32, 0.3, 1.7)
    blocks = SEQUENCE_LENGTH // POS_DEV
    multiplier = jnp.exp(jax.random.uniform(random_keys[2], (SEQS, blocks, 1), jnp.float32, 0.0, math.log(4.0))) * 0.5
    multiplier = jnp.repeat(multiplier, POS_DEV, axis=1)
    forget_speed = jnp.where(sluggish_heads, slow_rate / SEQUENCE_LENGTH, 1.0 / 40.0)
    spike_events = (jax.random.uniform(random_keys[3], tensor_extent, jnp.float32) < 2.0 / SEQUENCE_LENGTH) & sluggish_heads
    spike_depth = jax.random.uniform(random_keys[4], tensor_extent, jnp.float32, 0.22, 0.7)
    quick_events = (jax.random.uniform(random_keys[5], tensor_extent, jnp.float32) < 1.0 / 16.0) & jnp.logical_not(sluggish_heads)
    quick_depth = jax.random.uniform(random_keys[6], tensor_extent, jnp.float32, 1.0, 3.0)
    gate_logarithm = -(forget_speed * jaggedness * multiplier + jnp.where(spike_events, spike_depth, 0.0) + jnp.where(quick_events, quick_depth, 0.0))
    return jnp.cumsum(gate_logarithm, axis=1).astype(jnp.float32)


def block_levels(own_key, dims, cuts, least, high):
    gain, own = 1.0, jax.random.fold_in(own_key, 6)
    for position, blocks in cuts:
        heights = jnp.exp(jax.random.uniform(jax.random.fold_in(own, position), (blocks,), jnp.float32, least / len(cuts), high / len(cuts)))
        gain = gain * jnp.repeat(heights, dims[position] // blocks).reshape([-1 if axis == position else 1 for axis in range(len(dims))])
    return gain


def noise(rng, extent, scale, bound, cuts=(), kind=jnp.bfloat16):
    array = scale * jax.random.normal(rng, extent, jnp.float32)
    if cuts:
        array = array * block_levels(rng, extent, cuts, -0.22, 0.18)
    return jnp.clip(array, -bound, bound).astype(kind)


def setup_inputs(seed: int = 0) -> dict:
    keys = jax.random.split(jax.random.key(seed), 7)
    return {
        "hidden_states": draw_hidden_states(jax.random.fold_in(keys[6], 71), 0),
        "cumulative_gate": draw_cumulative_gate(jax.random.fold_in(keys[6], 71), 0),
        "query_weight": noise(keys[2], (D, QW), D ** -0.5, 0.125, ((0, 8),)),
        "key_weight": noise(keys[3], (D, KVW), D ** -0.5, 0.125, ((0, 8),)),
        "value_weight": noise(keys[4], (D, KVW), D ** -0.5, 0.125, ((0, 8),)),
        "out_weight": noise(keys[5], (QW, D), (QW // 32) ** -0.5, 0.75, ((0, 8),)),
    }


def attend_one(query_head, key_head, value_head, gate_head):
    length = query_head.shape[0]
    block_rows = math.gcd(length, 512)
    block_count = length // block_rows
    key_index = jnp.arange(length, dtype=jnp.int32)
    scaling = query_head.shape[1] ** -0.5

    def one_block(block_number):
        offset = (block_number * block_rows).astype(jnp.int32)
        query_block = lax.dynamic_slice_in_dim(query_head, offset, block_rows, 0)
        gate_block = lax.dynamic_slice_in_dim(gate_head, offset, block_rows, 0)
        scores = jnp.dot(query_block, key_head.T, preferred_element_type=jnp.float32) * scaling
        scores = scores + gate_block[:, None] - gate_head[None, :]
        row_index = offset + jnp.arange(block_rows, dtype=jnp.int32)
        allowed = key_index[None, :] <= row_index[:, None]
        scores = jnp.where(allowed, scores, -jnp.inf)
        maximum = jnp.max(scores, axis=1, keepdims=True)
        exponent = jnp.where(allowed, jnp.exp(scores - maximum), 0.0)
        weights = (exponent / jnp.sum(exponent, axis=1, keepdims=True)).astype(jnp.bfloat16)
        return jnp.dot(weights, value_head, preferred_element_type=jnp.float32).astype(jnp.bfloat16)

    result = lax.map(one_block, jnp.arange(block_count, dtype=jnp.int32))
    return result.reshape(length, query_head.shape[1])


def reference(hidden_states, cumulative_gate, query_weight, key_weight, value_weight, out_weight):
    flattened = hidden_states.reshape(SEQS * SEQUENCE_LENGTH, D)
    query = jnp.dot(flattened, query_weight, preferred_element_type=jnp.float32).astype(jnp.bfloat16)
    query = query.reshape(SEQS, SEQUENCE_LENGTH, HEADS, HEAD)
    key = jnp.dot(flattened, key_weight, preferred_element_type=jnp.float32).astype(jnp.bfloat16)
    key = key.reshape(SEQS, SEQUENCE_LENGTH, KV_HEADS, HEAD)
    value = jnp.dot(flattened, value_weight, preferred_element_type=jnp.float32).astype(jnp.bfloat16)
    value = value.reshape(SEQS, SEQUENCE_LENGTH, KV_HEADS, HEAD)
    group_size = HEADS // KV_HEADS

    def per_sequence(inputs):
        seq_query, seq_key, seq_value, seq_gate = inputs

        def per_head(head_number):
            shared = head_number // group_size
            return attend_one(seq_query[:, head_number], seq_key[:, shared], seq_value[:, shared], seq_gate[:, head_number])

        return lax.map(per_head, jnp.arange(HEADS, dtype=jnp.int32))

    attended = lax.map(per_sequence, (query, key, value, cumulative_gate))
    attended = jnp.transpose(attended, (0, 2, 1, 3)).reshape(SEQS * SEQUENCE_LENGTH, QW)
    mixed = jnp.dot(attended, out_weight, preferred_element_type=jnp.float32).astype(jnp.bfloat16)
    return mixed.reshape(SEQS, SEQUENCE_LENGTH, D)
```

```python
import functools

import jax
import jax.numpy as jnp
from jax import lax
from jax.experimental import pallas as pl
from jax.experimental.pallas import tpu as pltpu
from jax.sharding import Mesh
from jax.sharding import PartitionSpec as P

Z, Y, X, C = 8, 4, 4, 2
GROUPS = 8
HEAD = 64
POS = 128
BLOCKS = 32
LENGTH = BLOCKS * POS
TILE = 512
NEG = -1e30


def shift(value, axis, size, by):
    return lax.ppermute(value, axis, [(i, (i + by) % size) for i in range(size)])


def swap(value):
    return lax.ppermute(value, "c", [(0, 1), (1, 0)])


def gather_x(own):
    half = own.shape[0] // 2
    before = shift(own, "x", X, 1)
    after = shift(own, "x", X, -1)
    far_low = shift(before[:half], "x", X, 1)
    far_high = shift(after[half:], "x", X, -1)
    return own, before, after, far_low, far_high


def project_kernel(where_ref, own_ref, other_ref, w0, w1, w2, w3, w4, out_ref):
    x = where_ref[0]
    c = where_ref[1]
    chips = (x, lax.rem(x + 3, 4), lax.rem(x + 1, 4), lax.rem(x + 2, 4))
    pieces = []
    for chip, ref, row, flip in (
        (chips[0], w0, 0, 0), (chips[0], w0, 256, 1),
        (chips[1], w1, 0, 0), (chips[1], w1, 256, 1),
        (chips[2], w2, 0, 0), (chips[2], w2, 256, 1),
        (chips[3], w3, 0, 0), (chips[3], w4, 0, 1),
    ):
        column = (chip * 2 + (c if flip == 0 else 1 - c)) * 256
        pieces.append((pl.multiple_of(column, 256), ref, row))
    for tokens_ref, base in ((own_ref, c * 2), (other_ref, 2 - c * 2)):
        for n in range(6):
            total = None
            for column, ref, row in pieces:
                part = jnp.dot(
                    tokens_ref[:, pl.ds(column, 256)],
                    ref[row : row + 256, n * 256 : n * 256 + 256],
                    preferred_element_type=jnp.float32,
                )
                total = part if total is None else total + part
            if n < 4:
                total = total * 0.125
            for s in range(2):
                flipped = total[s * 128 : s * 128 + 128].T.astype(jnp.bfloat16)
                unit = (base + s) * GROUPS
                if n < 4:
                    for k in range(2):
                        out_ref[unit + 2 * n + k, 0:128, :] = flipped[k * 128 : k * 128 + 128]
                else:
                    for k in range(4):
                        out_ref[unit + 4 * (n - 4) + k, 128:192, :] = flipped[k * 64 : k * 64 + 64]


def project(where, own, other, weights):
    vmem = pl.BlockSpec(memory_space=pltpu.VMEM)
    return pl.pallas_call(
        project_kernel,
        out_shape=jax.ShapeDtypeStruct((BLOCKS, 192, POS), jnp.bfloat16),
        in_specs=[pl.BlockSpec(memory_space=pltpu.SMEM)] + [vmem] * 7,
        out_specs=vmem,
        cost_estimate=pl.CostEstimate(
            flops=2 * 512 * 2048 * 1536, bytes_accessed=10 << 20, transcendentals=0
        ),
        name="project",
    )(where, own, other, *weights)


def attend_kernel(where_ref, qkv_ref, kv_ref, gate_ref, out_ref, keys, values, top, total):
    i = pl.program_id(0)
    per = TILE // POS

    @pl.when(i == 0)
    def _():
        row = lax.broadcasted_iota(jnp.int32, (64, POS), 0)

        def one(j, _):
            mine = qkv_ref[j, 128:192, :]
            theirs = kv_ref[j]
            first = where_ref[1] == 0
            key = jnp.where(first, mine, theirs)
            value = jnp.where(first, theirs, mine)
            minus = -gate_ref[j]
            high = minus.astype(jnp.bfloat16).astype(jnp.float32)
            rest = minus - high
            middle = rest.astype(jnp.bfloat16).astype(jnp.float32)
            low = rest - middle
            extra = jnp.zeros((64, POS), jnp.float32)
            for h in range(2):
                for k, part in enumerate((high, middle, low)):
                    extra = jnp.where(row == 3 * h + k, part[h : h + 1], extra)
            whole = jnp.concatenate([key.astype(jnp.float32), extra], axis=0)
            at = pl.multiple_of(j * POS, POS)
            keys[pl.ds(at, POS), :] = whole.T.astype(jnp.bfloat16)
            ones = jnp.where(row[:16] == 0, 1.0, 0.0).astype(jnp.bfloat16)
            values[0:64, pl.ds(at, POS)] = value
            values[64:80, pl.ds(at, POS)] = ones
            return 0

        lax.fori_loop(0, BLOCKS, one, 0)

    row = lax.broadcasted_iota(jnp.int32, (64, TILE), 0)
    queries = []
    for h in range(2):
        parts = [qkv_ref[i * per + b, h * 64 : h * 64 + 64, :] for b in range(per)]
        ones = jnp.where((row >= 3 * h) & (row < 3 * h + 3), 1.0, 0.0).astype(jnp.bfloat16)
        queries.append(jnp.concatenate([jnp.concatenate(parts, axis=1), ones], axis=0))

    def step(j, masked):
        at = pl.multiple_of(j * TILE, TILE)
        block_keys = keys[pl.ds(at, TILE), :]
        block_values = values[:, pl.ds(at, TILE)]
        for h in range(2):
            scores = jnp.dot(block_keys, queries[h], preferred_element_type=jnp.float32)
            if masked:
                s = lax.broadcasted_iota(jnp.int32, (TILE, TILE), 0)
                t = lax.broadcasted_iota(jnp.int32, (TILE, TILE), 1)
                scores = jnp.where(s <= t, scores, NEG)
            before = top[h]
            now = jnp.maximum(before, jnp.max(scores, axis=0, keepdims=True))
            top[h] = now
            weights = jnp.exp(scores - now).astype(jnp.bfloat16)
            total[h] = total[h] * jnp.exp(before - now) + jnp.dot(
                block_values, weights, preferred_element_type=jnp.float32
            )

    top[...] = jnp.full(top.shape, NEG, jnp.float32)
    total[...] = jnp.zeros(total.shape, jnp.float32)

    def body(j, _):
        step(j, False)
        return 0

    lax.fori_loop(0, i, body, 0)
    step(i, True)
    for h in range(2):
        result = (total[h, 0:64] / total[h, 64:65]).astype(jnp.bfloat16)
        for b in range(per):
            out_ref[b, h * 64 : h * 64 + 64, :] = result[:, b * POS : b * POS + POS]


def attend(where, qkv, kv, gates):
    vmem = pl.BlockSpec(memory_space=pltpu.VMEM)
    per = TILE // POS
    return pl.pallas_call(
        attend_kernel,
        grid=(LENGTH // TILE,),
        out_shape=jax.ShapeDtypeStruct((BLOCKS, 128, POS), jnp.bfloat16),
        in_specs=[pl.BlockSpec(memory_space=pltpu.SMEM)] + [vmem] * 3,
        out_specs=pl.BlockSpec((per, 128, POS), lambda i: (i, 0, 0)),
        scratch_shapes=[
            pltpu.VMEM((LENGTH, 128), jnp.bfloat16),
            pltpu.VMEM((80, LENGTH), jnp.bfloat16),
            pltpu.VMEM((2, 1, TILE), jnp.float32),
            pltpu.VMEM((2, 80, TILE), jnp.float32),
        ],
        compiler_params=pltpu.CompilerParams(dimension_semantics=("arbitrary",)),
        cost_estimate=pl.CostEstimate(
            flops=2 * 2 * 2 * LENGTH * LENGTH * 128, bytes_accessed=4 << 20,
            transcendentals=LENGTH * LENGTH,
        ),
        name="attend",
    )(where, qkv, kv, gates)


def on_device(hidden, gate, wq, wk, wv, wo):
    x = lax.axis_index("x")
    c = lax.axis_index("c")
    where = jnp.stack([x, c]).astype(jnp.int32)
    own = hidden.reshape(256, 2048)
    other = swap(own)

    wq = wq.reshape(256, GROUPS, 2, 128)
    first = jnp.concatenate([wq[:, :, 0].reshape(256, 1024), wk], axis=1)
    second = jnp.concatenate([wq[:, :, 1].reshape(256, 1024), wv], axis=1)
    keep = jnp.where(c == 0, first, second)
    give = jnp.where(c == 0, second, first)
    shard = jnp.concatenate([keep, swap(give)], axis=0)
    weights = gather_x(shard)

    by_unit = gate.reshape(2, POS, GROUPS, 2, 2)
    by_unit = jnp.transpose(by_unit, (3, 0, 2, 4, 1))
    keep = jnp.where(c == 0, by_unit[0], by_unit[1])
    got = swap(jnp.where(c == 0, by_unit[1], by_unit[0]))
    gates = jnp.where(c == 0, jnp.stack([keep, got]), jnp.stack([got, keep]))
    gates = gates.reshape(BLOCKS, 2, POS)
    gates = lax.all_to_all(gates, ("z", "y"), 0, 0, tiled=True)

    qkv = project(where, own, other, weights)
    qkv = lax.all_to_all(qkv, ("z", "y"), 0, 0, tiled=True)
    kv = swap(qkv[:, 128:192])

    wo, _ = lax.optimization_barrier((wo, weights[4]))
    wo = wo.reshape(2, 128, 2048)
    keep = jnp.where(c == 0, wo[0], wo[1])
    got = swap(jnp.where(c == 0, wo[1], wo[0]))
    shard = jnp.where(c == 0, jnp.concatenate([keep, got]), jnp.concatenate([got, keep]))
    o0, o1, o2, o3, o4 = gather_x(shard)

    attended = attend(where, qkv, kv, gates)
    back = lax.all_to_all(attended, ("z", "y"), 0, 0, tiled=True)
    back = back.reshape(4, X, 256, POS)
    total = None
    for by, block in ((0, o0), (3, o1), (1, o2), (2, jnp.concatenate([o3, o4]))):
        piece = lax.dynamic_index_in_dim(back, lax.rem(x + by, X), 1, keepdims=False)
        part = lax.dot_general(
            piece, block, (((1,), (0,)), ((), ())), preferred_element_type=jnp.float32
        )
        total = part if total is None else total + part
    total = total.reshape(2, 2, POS, 2048)
    mine = lax.dynamic_index_in_dim(total, c, 0, keepdims=False)
    theirs = lax.dynamic_index_in_dim(total, 1 - c, 0, keepdims=False)
    mixed = mine + swap(theirs.astype(jnp.bfloat16)).astype(jnp.float32)
    return mixed.astype(jnp.bfloat16)


def solution(mesh):
    mesh = Mesh(mesh.devices.reshape(Z, Y, X, C), ("z", "y", "x", "c"))
    dp, sp = ("x", "c"), ("z", "y")
    placed = (P(dp, sp, None), P(dp, sp, None), P(dp, None), P(dp, None), P(dp, None), P(dp, None))
    return jax.shard_map(
        on_device, mesh=mesh, in_specs=placed, out_specs=P(dp, sp, None), check_vma=False
    )
```

```python
import functools

import jax
import jax.numpy as jnp
from jax import lax
from jax.experimental import pallas as pl
from jax.experimental.pallas import tpu as pltpu
from jax.sharding import Mesh
from jax.sharding import PartitionSpec as P

Z, X = 8, 4
GROUPS = 8
POS = 128
BLOCKS = 32
UNITS = 16
LENGTH = BLOCKS * POS
TILE = 512
PART = 256
NEG = -1e30
VMEM = pl.BlockSpec(memory_space=pltpu.VMEM)
SMEM = pl.BlockSpec(memory_space=pltpu.SMEM)


def shift(value, by):
    return lax.ppermute(value, "x", [(i, (i + by) % X) for i in range(X)])


def swap(value, axis="core"):
    return lax.ppermute(value, axis, [(0, 1), (1, 0)])


def exchange(value, axes):
    return lax.all_to_all(value, axes, 0, 0, tiled=True)


def gather_x(own):
    half = own.shape[0] // 2
    before = shift(own, 1)
    after = shift(own, -1)
    low = shift(before[:half], 1)
    high = shift(after[half:], -1)
    return own, before, after, low, high


def fetch_x(own):
    return (own, shift(own, 1), shift(own, -1), shift(own, 2))


def call(kernel, flops, mebibytes=16, **arguments):
    return pl.pallas_call(
        kernel,
        compiler_params=pltpu.CompilerParams(vmem_limit_bytes=mebibytes << 20),
        cost_estimate=pl.CostEstimate(flops=flops, bytes_accessed=4 << 20, transcendentals=0),
        **arguments,
    )


def arrange_kernel(where_ref, query_ref, keep, give):
    c = where_ref[1]
    p = where_ref[2]
    first = c == 0
    for g in range(4):
        at = pl.multiple_of(p * 1024 + g * 256, 256)
        low = query_ref[:, pl.ds(at, 128)]
        high = query_ref[:, pl.ds(at + 128, 128)]
        keep[:, g * 128 : g * 128 + 128] = jnp.where(first, low, high)
        give[:, g * 128 : g * 128 + 128] = jnp.where(first, high, low)


def arrange(where, wq):
    shape = jax.ShapeDtypeStruct((256, 512), jnp.bfloat16)
    return call(
        arrange_kernel, 1 << 20, out_shape=(shape,) * 2,
        in_specs=[SMEM, VMEM], out_specs=(VMEM,) * 2,
    )(where, wq)


def pieces_of(where_ref, refs):
    x = where_ref[0]
    c = where_ref[1]
    pieces = []
    for step, ref, flips in zip((0, 3, 1, 2, 2), refs, ((0, 1), (0, 1), (0, 1), (0, 1), (1,))):
        for flip in flips[: ref.shape[0] // 256]:
            column = (lax.rem(x + step, X) * 2 + (1 - c if flip else c)) * 256
            pieces.append((pl.multiple_of(column, 256), ref, 256 * (len(flips) - 1) * flip))
    return pieces


def product(tokens, pieces, columns):
    total = None
    for column, ref, row in pieces:
        part = jnp.dot(
            tokens[:, pl.ds(column, 256)], ref[row : row + 256, columns],
            preferred_element_type=jnp.float32,
        )
        total = part if total is None else total + part
    return total


def project_kv_kernel(where_ref, t0, t1, gate_ref, w0, w1, w2, w3, w4, out_ref):
    c = where_ref[1]
    pieces = pieces_of(where_ref, (w0, w1, w2, w3, w4))
    row = lax.broadcasted_iota(jnp.int32, (16, POS), 0)
    for ref, core in ((t0, c), (t1, 1 - c)):
        for p in range(2):
            total = product(ref, pieces, slice(p * 256, p * 256 + 256))
            for s in range(2):
                flipped = total[s * POS : s * POS + POS].T.astype(jnp.bfloat16)
                for g in range(4):
                    unit = (core * 2 + s) * GROUPS + g * 2 + p
                    out_ref[unit, 0:64] = flipped[g * 64 : g * 64 + 64]
    for u in range(BLOCKS):
        minus = -gate_ref[u]
        high = minus.astype(jnp.bfloat16).astype(jnp.float32)
        rest = minus - high
        middle = rest.astype(jnp.bfloat16).astype(jnp.float32)
        low = rest - middle
        extra = jnp.zeros((16, POS), jnp.float32)
        for h in range(2):
            for k, part in enumerate((high, middle, low)):
                extra = jnp.where(row == 3 * h + k, part[h : h + 1], extra)
        out_ref[u, 64:80] = extra.astype(jnp.bfloat16)


def project_kv(where, tokens, gates, weights):
    return call(
        project_kv_kernel, 2 * 512 * 2048 * 512,
        out_shape=jax.ShapeDtypeStruct((BLOCKS, 80, POS), jnp.bfloat16),
        in_specs=[SMEM] + [VMEM] * 8, out_specs=VMEM,
    )(where, *tokens, gates, *weights)


def project_q_kernel(where_ref, t0, t1, t2, t3, w0, w1, w2, w3, out_ref):
    c = where_ref[1]
    p = where_ref[2]
    pieces = pieces_of(where_ref, (w0, w1, w2, w3))
    for ref, core, side in ((t0, c, p), (t1, 1 - c, p), (t2, c, 1 - p), (t3, 1 - c, 1 - p)):
        at = pl.multiple_of(side * POS, POS)
        for n in range(2):
            total = product(ref, pieces, slice(n * 256, n * 256 + 256)) * 0.125
            for s in range(2):
                flipped = total[s * POS : s * POS + POS].T.astype(jnp.bfloat16)
                unit = (core * 2 + s) * 4 + n * 2
                for k in range(2):
                    out_ref[unit + k, :, pl.ds(at, POS)] = flipped[k * 128 : k * 128 + 128]


def project_q(where, tokens, weights):
    return call(
        project_q_kernel, 2 * 1024 * 2048 * 512,
        out_shape=jax.ShapeDtypeStruct((UNITS, 128, 2 * POS), jnp.bfloat16),
        in_specs=[SMEM] + [VMEM] * 8, out_specs=VMEM,
    )(where, *tokens, *weights)


def attend_kernel(
    where_ref, q_ref, mine_ref, theirs_ref, out_ref,
    keys, values, query, scores, peak, top, total,
):
    blocks = LENGTH // TILE
    per = TILE // POS
    first = where_ref[1] == 0
    row = lax.broadcasted_iota(jnp.int32, (16, POS), 0)
    ones = jnp.where(row == 0, 1.0, 0.0).astype(jnp.bfloat16)
    rest = jnp.zeros((48, POS), jnp.bfloat16)
    for j in range(BLOCKS):
        mine = mine_ref[j, 0:64]
        theirs = theirs_ref[j]
        key = jnp.where(first, mine, theirs)
        whole = jnp.concatenate([key, mine_ref[j, 64:80], rest], axis=0)
        at = slice(j * POS, j * POS + POS)
        keys[at, :] = whole.astype(jnp.float32).T.astype(jnp.bfloat16)
        values[0:64, at] = jnp.where(first, theirs, mine)
        values[64:80, at] = ones
    row = lax.broadcasted_iota(jnp.int32, (64, 2 * POS), 0)
    for h in range(2):
        ones = jnp.where((row >= 3 * h) & (row < 3 * h + 3), 1.0, 0.0).astype(jnp.bfloat16)
        for b in range(UNITS):
            at = slice(b * 2 * POS, b * 2 * POS + 2 * POS)
            query[h, 0:64, at] = q_ref[b, h * 64 : h * 64 + 64]
            query[h, 64:128, at] = ones

    def score(h, i, j, slot, diagonal, r):
        s = jnp.dot(
            keys[pl.ds(pl.multiple_of(j * TILE + r * PART, PART), PART), :],
            query[h, :, pl.ds(pl.multiple_of(i * TILE, TILE), TILE)],
            preferred_element_type=jnp.float32,
        )
        if diagonal:
            a = lax.broadcasted_iota(jnp.int32, (PART, TILE), 0)
            b = lax.broadcasted_iota(jnp.int32, (PART, TILE), 1)
            s = jnp.where(a + r * PART <= b, s, NEG)
        scores[slot, r * PART : r * PART + PART] = s
        m = jnp.max(s, axis=0, keepdims=True)
        peak[slot] = m if r == 0 else jnp.maximum(peak[slot], m)

    def begin(j, slot):
        before = jnp.where(j == 0, NEG, top[...])
        now = jnp.maximum(before, peak[slot])
        top[...] = now
        total[...] = total[...] * jnp.exp(before - now)

    def add(j, slot, r):
        p = jnp.exp(scores[slot, r * PART : r * PART + PART] - top[...]).astype(jnp.bfloat16)
        total[...] += jnp.dot(
            values[:, pl.ds(pl.multiple_of(j * TILE + r * PART, PART), PART)], p,
            preferred_element_type=jnp.float32,
        )

    def finish(h, i):
        result = (total[0:64] / total[64:65]).astype(jnp.bfloat16)
        row = pl.multiple_of(h * 64, 64)
        for b in range(per):
            out_ref[i * per + b, pl.ds(row, 64), :] = result[:, b * POS : b * POS + POS]

    total[...] = jnp.zeros(total.shape, jnp.float32)
    top[...] = jnp.full(top.shape, NEG, jnp.float32)
    for r in range(TILE // PART):
        score(0, 0, 0, 0, True, r)

    def one(h, i, j, slot):
        last = j == i
        over = last & (i == blocks - 1)
        later_h = jnp.where(over, h + 1, h)
        later_i = jnp.where(over, 0, jnp.where(last, i + 1, i))
        later_j = jnp.where(last, 0, j + 1)
        safe_h = jnp.minimum(later_h, 1)

        def go(diagonal):
            begin(j, slot)
            for r in range(TILE // PART):
                score(safe_h, later_i, later_j, 1 - slot, diagonal, r)
                add(j, slot, r)

        @pl.when(later_i == later_j)
        def _():
            go(True)

        @pl.when(later_i != later_j)
        def _():
            go(False)

        @pl.when(last)
        def _():
            finish(h, i)

        return later_h, later_i, later_j

    def two(_, carry):
        return one(*one(*carry, 0), 1)

    zero = jnp.int32(0)
    lax.fori_loop(0, blocks * (blocks + 1) // 2, two, (zero, zero, zero))


def attend(where, query, mine, theirs):
    return call(
        attend_kernel, 4 * LENGTH * LENGTH * 256,
        out_shape=jax.ShapeDtypeStruct((BLOCKS, 128, POS), jnp.bfloat16),
        in_specs=[SMEM] + [VMEM] * 3, out_specs=VMEM,
        scratch_shapes=[
            pltpu.VMEM((LENGTH, 128), jnp.bfloat16),
            pltpu.VMEM((80, LENGTH), jnp.bfloat16),
            pltpu.VMEM((2, 128, LENGTH), jnp.bfloat16),
            pltpu.VMEM((2, TILE, TILE), jnp.float32),
            pltpu.VMEM((2, 1, TILE), jnp.float32),
            pltpu.VMEM((1, TILE), jnp.float32),
            pltpu.VMEM((80, TILE), jnp.float32),
        ],
    )(where, query, mine, theirs)


def mix_kernel(own, where_ref, back, w0, w1, w2, w3, out_ref, left):
    x = where_ref[0]
    c = where_ref[1]
    base = 2 * (c if own else 1 - c)

    @pl.when(pl.program_id(0) == 0)
    def _():
        for k, step in enumerate((0, 3, 1, 2)):
            chip = lax.rem(x + step, X)
            for s in range(2):
                unit = (base + s) * GROUPS + lax.rem(chip, 2) * 4 + lax.div(chip, 2)
                block = jnp.concatenate([back[unit], back[unit + 2]], axis=0)
                block = block.astype(jnp.float32).T.astype(jnp.bfloat16)
                left[k, s * POS : s * POS + POS] = block

    total = None
    for k, ref in enumerate((w0, w1, w2, w3)):
        part = jnp.dot(left[k], ref[...], preferred_element_type=jnp.float32)
        total = part if total is None else total + part
    out_ref[...] = total.astype(out_ref.dtype)


def mix(own, where, back, weights):
    part = pl.BlockSpec((256, 512), lambda n: (0, n))
    return call(
        functools.partial(mix_kernel, own), 2 * 256 * 1024 * 2048,
        grid=(4,),
        out_shape=jax.ShapeDtypeStruct((256, 2048), jnp.float32 if own else jnp.bfloat16),
        in_specs=[SMEM, VMEM] + [part] * 4, out_specs=part,
        scratch_shapes=[pltpu.VMEM((4, 256, 256), jnp.bfloat16)],
    )(where, back, *weights)


def after(value, *others):
    return lax.optimization_barrier((value, *others))[0]


def layer(hidden, gate, wq, wk, wv, wo):
    x = lax.axis_index("x")
    c = lax.axis_index("core")
    first = c == 0
    where = jnp.stack([x, c, lax.axis_index("yl")]).astype(jnp.int32)
    own = hidden.reshape(256, 2048)
    homes = ("z", "yh", "yl")

    beside = swap(own, "yl")
    shard = jnp.concatenate([jnp.where(first, wk, wv), swap(jnp.where(first, wv, wk))], axis=0)
    kv_weights = gather_x(shard)
    keep, give = arrange(where, wq)
    shard = jnp.concatenate([keep, swap(give)], axis=0)
    q_weights = fetch_x(after(shard, kv_weights[1], kv_weights[2]))
    other = swap(own)

    by_unit = jnp.transpose(gate.reshape(2, POS, 2, 4, 2, 2), (4, 0, 3, 2, 5, 1))
    mine = jnp.where(first, by_unit[0], by_unit[1])
    got = swap(jnp.where(first, by_unit[1], by_unit[0]))
    gates = jnp.where(first, jnp.stack([mine, got]), jnp.stack([got, mine]))
    gates = gates.reshape(BLOCKS, 2, POS)

    kv = project_kv(where, (own, other), gates, kv_weights)
    kv = exchange(kv, homes)
    tokens = (own, other, beside, swap(beside))
    query = project_q(where, tokens, q_weights)
    theirs = swap(kv[:, :64])
    query = exchange(query, ("z", "yh"))

    halves = wo.reshape(2, 128, 2048)
    mine = jnp.where(first, halves[0], halves[1])
    got = swap(jnp.where(first, halves[1], halves[0]))
    shard = jnp.where(first, jnp.concatenate([mine, got]), jnp.concatenate([got, mine]))
    o_weights = fetch_x(after(shard, *q_weights[1:]))

    back = exchange(attend(where, query, kv, theirs), homes)
    theirs = swap(mix(False, where, back, o_weights))
    mine = mix(True, where, back, o_weights)
    mixed = mine + theirs.astype(jnp.float32)
    return mixed.astype(jnp.bfloat16).reshape(2, POS, 2048)


def solution(mesh):
    fine = Mesh(mesh.devices.reshape(Z, 2, 2, X, 2), ("z", "yh", "yl", "x", "core"))
    dp, sp = ("x", "core"), ("z", "yh", "yl")
    placed = (P(dp, sp, None), P(dp, sp, None), P(dp, None), P(dp, None), P(dp, None), P(dp, None))
    return jax.shard_map(
        layer, mesh=fine, in_specs=placed, out_specs=P(dp, sp, None), check_vma=False
    )
```

```python
import functools

import jax
import jax.numpy as jnp
from jax import lax
from jax.experimental import pallas as pl
from jax.experimental.pallas import tpu as pltpu
from jax.sharding import Mesh
from jax.sharding import PartitionSpec as P

Z, X = 8, 4
GROUPS = 8
POS = 128
BLOCKS = 32
UNITS = 16
LENGTH = BLOCKS * POS
TILE = 1024
PART = 256
NEG = -1e30
VMEM = pl.BlockSpec(memory_space=pltpu.VMEM)
SMEM = pl.BlockSpec(memory_space=pltpu.SMEM)


def shift(value, by):
    return lax.ppermute(value, "x", [(i, (i + by) % X) for i in range(X)])


def swap(value, axis="core"):
    return lax.ppermute(value, axis, [(0, 1), (1, 0)])


def exchange(value, axes):
    return lax.all_to_all(value, axes, 0, 0, tiled=True)


def gather_x(own):
    half = own.shape[0] // 2
    before = shift(own, 1)
    after = shift(own, -1)
    low = shift(before[:half], 1)
    high = shift(after[half:], -1)
    return own, before, after, low, high


def fetch_x(own):
    return (own, shift(own, 1), shift(own, -1), shift(own, 2))


def call(kernel, flops, mebibytes=16, **arguments):
    return pl.pallas_call(
        kernel,
        compiler_params=pltpu.CompilerParams(vmem_limit_bytes=mebibytes << 20),
        cost_estimate=pl.CostEstimate(flops=flops, bytes_accessed=4 << 20, transcendentals=0),
        **arguments,
    )


def arrange_kernel(where_ref, query_ref, keep, give):
    c = where_ref[1]
    p = where_ref[2]
    first = c == 0
    for g in range(4):
        at = pl.multiple_of(p * 1024 + g * 256, 256)
        low = query_ref[:, pl.ds(at, 128)]
        high = query_ref[:, pl.ds(at + 128, 128)]
        keep[:, g * 128 : g * 128 + 128] = jnp.where(first, low, high)
        give[:, g * 128 : g * 128 + 128] = jnp.where(first, high, low)


def arrange(where, wq):
    shape = jax.ShapeDtypeStruct((256, 512), jnp.bfloat16)
    return call(
        arrange_kernel, 1 << 20, out_shape=(shape,) * 2,
        in_specs=[SMEM, VMEM], out_specs=(VMEM,) * 2,
    )(where, wq)


def pieces_of(where_ref, refs):
    x = where_ref[0]
    c = where_ref[1]
    pieces = []
    for step, ref, flips in zip((0, 3, 1, 2, 2), refs, ((0, 1), (0, 1), (0, 1), (0, 1), (1,))):
        for flip in flips[: ref.shape[0] // 256]:
            column = (lax.rem(x + step, X) * 2 + (1 - c if flip else c)) * 256
            pieces.append((pl.multiple_of(column, 256), ref, 256 * (len(flips) - 1) * flip))
    return pieces


def product(tokens, pieces, columns):
    total = None
    for column, ref, row in pieces:
        part = jnp.dot(
            tokens[:, pl.ds(column, 256)], ref[row : row + 256, columns],
            preferred_element_type=jnp.float32,
        )
        total = part if total is None else total + part
    return total


def project_kv_kernel(where_ref, t0, t1, gate_ref, w0, w1, w2, w3, w4, out_ref):
    c = where_ref[1]
    pieces = pieces_of(where_ref, (w0, w1, w2, w3, w4))
    row = lax.broadcasted_iota(jnp.int32, (16, POS), 0)
    for ref, core in ((t0, c), (t1, 1 - c)):
        for p in range(2):
            total = product(ref, pieces, slice(p * 256, p * 256 + 256))
            for s in range(2):
                flipped = total[s * POS : s * POS + POS].T.astype(jnp.bfloat16)
                for g in range(4):
                    unit = (core * 2 + s) * GROUPS + g * 2 + p
                    out_ref[unit, 0:64] = flipped[g * 64 : g * 64 + 64]
    for u in range(BLOCKS):
        minus = -gate_ref[u]
        high = minus.astype(jnp.bfloat16).astype(jnp.float32)
        rest = minus - high
        middle = rest.astype(jnp.bfloat16).astype(jnp.float32)
        low = rest - middle
        extra = jnp.zeros((16, POS), jnp.float32)
        for h in range(2):
            for k, part in enumerate((high, middle, low)):
                extra = jnp.where(row == 3 * h + k, part[h : h + 1], extra)
        out_ref[u, 64:80] = extra.astype(jnp.bfloat16)


def project_kv(where, tokens, gates, weights):
    return call(
        project_kv_kernel, 2 * 512 * 2048 * 512,
        out_shape=jax.ShapeDtypeStruct((BLOCKS, 80, POS), jnp.bfloat16),
        in_specs=[SMEM] + [VMEM] * 8, out_specs=VMEM,
    )(where, *tokens, gates, *weights)


def project_q_kernel(where_ref, t0, t1, t2, t3, w0, w1, w2, w3, out_ref):
    c = where_ref[1]
    p = where_ref[2]
    pieces = pieces_of(where_ref, (w0, w1, w2, w3))
    for ref, core, side in ((t0, c, p), (t1, 1 - c, p), (t2, c, 1 - p), (t3, 1 - c, 1 - p)):
        at = pl.multiple_of(side * POS, POS)
        for n in range(2):
            total = product(ref, pieces, slice(n * 256, n * 256 + 256)) * 0.125
            for s in range(2):
                flipped = total[s * POS : s * POS + POS].T.astype(jnp.bfloat16)
                unit = (core * 2 + s) * 4 + n * 2
                for k in range(2):
                    out_ref[unit + k, :, pl.ds(at, POS)] = flipped[k * 128 : k * 128 + 128]


def project_q(where, tokens, weights):
    return call(
        project_q_kernel, 2 * 1024 * 2048 * 512,
        out_shape=jax.ShapeDtypeStruct((UNITS, 128, 2 * POS), jnp.bfloat16),
        in_specs=[SMEM] + [VMEM] * 8, out_specs=VMEM,
    )(where, *tokens, *weights)


def attend_kernel(
    where_ref, q_ref, mine_ref, theirs_ref, out_ref,
    keys, values, query, scores, peak, top, total,
):
    blocks = LENGTH // TILE
    per = TILE // POS
    first = where_ref[1] == 0
    row = lax.broadcasted_iota(jnp.int32, (16, POS), 0)
    ones = jnp.where(row == 0, 1.0, 0.0).astype(jnp.bfloat16)
    rest = jnp.zeros((48, POS), jnp.bfloat16)
    for j in range(BLOCKS):
        mine = mine_ref[j, 0:64]
        theirs = theirs_ref[j]
        key = jnp.where(first, mine, theirs)
        whole = jnp.concatenate([key, mine_ref[j, 64:80], rest], axis=0)
        at = slice(j * POS, j * POS + POS)
        keys[at, :] = whole.astype(jnp.float32).T.astype(jnp.bfloat16)
        values[0:64, at] = jnp.where(first, theirs, mine)
        values[64:80, at] = ones
    row = lax.broadcasted_iota(jnp.int32, (64, 2 * POS), 0)
    for h in range(2):
        ones = jnp.where((row >= 3 * h) & (row < 3 * h + 3), 1.0, 0.0).astype(jnp.bfloat16)
        for b in range(UNITS):
            at = slice(b * 2 * POS, b * 2 * POS + 2 * POS)
            query[h, 0:64, at] = q_ref[b, h * 64 : h * 64 + 64]
            query[h, 64:128, at] = ones

    def score(h, i, j, slot, diagonal, r):
        rows = slice(r * PART, r * PART + PART)
        skip = r * PART if diagonal else 0
        s = jnp.dot(
            keys[pl.ds(pl.multiple_of(j * TILE + r * PART, PART), PART), :],
            query[h, :, pl.ds(pl.multiple_of(i * TILE + skip, PART), TILE - skip)],
            preferred_element_type=jnp.float32,
        )
        if diagonal:
            a = lax.broadcasted_iota(jnp.int32, (PART, PART), 0)
            b = lax.broadcasted_iota(jnp.int32, (PART, PART), 1)
            near = jnp.where(a <= b, s[:, :PART], NEG)
            s = near if skip + PART == TILE else jnp.concatenate([near, s[:, PART:]], axis=1)
        scores[slot, rows, skip:] = s
        m = jnp.max(s, axis=0, keepdims=True)
        peak[slot, :, skip:] = m if r == 0 else jnp.maximum(peak[slot, :, skip:], m)

    def begin(j, slot):
        before = jnp.where(j == 0, NEG, top[...])
        now = jnp.maximum(before, peak[slot])
        top[...] = now
        total[...] = total[...] * jnp.exp(before - now)

    def add(j, slot, r, diagonal):
        skip = r * PART if diagonal else 0
        rows = slice(r * PART, r * PART + PART)
        p = jnp.exp(scores[slot, rows, skip:] - top[:, skip:]).astype(jnp.bfloat16)
        total[:, skip:] += jnp.dot(
            values[:, pl.ds(pl.multiple_of(j * TILE + r * PART, PART), PART)], p,
            preferred_element_type=jnp.float32,
        )

    def finish(h, i):
        result = (total[0:64] / total[64:65]).astype(jnp.bfloat16)
        row = pl.multiple_of(h * 64, 64)
        for b in range(per):
            out_ref[i * per + b, pl.ds(row, 64), :] = result[:, b * POS : b * POS + POS]

    total[...] = jnp.zeros(total.shape, jnp.float32)
    top[...] = jnp.full(top.shape, NEG, jnp.float32)
    for r in range(TILE // PART):
        score(0, 0, 0, 0, True, r)

    def one(h, i, j, slot):
        last = j == i
        over = last & (i == blocks - 1)
        later_h = jnp.where(over, h + 1, h)
        later_i = jnp.where(over, 0, jnp.where(last, i + 1, i))
        later_j = jnp.where(last, 0, j + 1)
        safe_h = jnp.minimum(later_h, 1)

        def go(diagonal, here):
            begin(j, slot)
            for r in range(TILE // PART):
                score(safe_h, later_i, later_j, 1 - slot, diagonal, r)
                add(j, slot, r, here)

        later = later_i == later_j

        @pl.when(later & last)
        def _():
            go(True, True)

        @pl.when(later & jnp.logical_not(last))
        def _():
            go(True, False)

        @pl.when(jnp.logical_not(later) & last)
        def _():
            go(False, True)

        @pl.when(jnp.logical_not(later | last))
        def _():
            go(False, False)

        @pl.when(last)
        def _():
            finish(h, i)

        return later_h, later_i, later_j

    def two(_, carry):
        return one(*one(*carry, 0), 1)

    zero = jnp.int32(0)
    lax.fori_loop(0, blocks * (blocks + 1) // 2, two, (zero, zero, zero))


def attend(where, query, mine, theirs):
    return call(
        attend_kernel, 4 * LENGTH * LENGTH * 256, 32,
        out_shape=pltpu.HBM((BLOCKS, 128, POS), jnp.bfloat16),
        in_specs=[SMEM] + [VMEM] * 3, out_specs=VMEM,
        scratch_shapes=[
            pltpu.VMEM((LENGTH, 128), jnp.bfloat16),
            pltpu.VMEM((80, LENGTH), jnp.bfloat16),
            pltpu.VMEM((2, 128, LENGTH), jnp.bfloat16),
            pltpu.VMEM((2, TILE, TILE), jnp.float32),
            pltpu.VMEM((2, 1, TILE), jnp.float32),
            pltpu.VMEM((1, TILE), jnp.float32),
            pltpu.VMEM((80, TILE), jnp.float32),
        ],
    )(where, query, mine, theirs)


def mix_kernel(own, where_ref, back, w0, w1, w2, w3, out_ref):
    x = where_ref[0]
    c = where_ref[1]
    base = 2 * (c if own else 1 - c)
    left = []
    for step in (0, 3, 1, 2):
        chip = lax.rem(x + step, X)
        rows = []
        for s in range(2):
            unit = (base + s) * GROUPS + lax.rem(chip, 2) * 4 + lax.div(chip, 2)
            block = jnp.concatenate([back[unit], back[unit + 2]], axis=0)
            rows.append(block.astype(jnp.float32).T.astype(jnp.bfloat16))
        left.append(jnp.concatenate(rows, axis=0))
    for n in range(8):
        at = slice(n * 256, n * 256 + 256)
        total = None
        for a, ref in zip(left, (w0, w1, w2, w3)):
            part = jnp.dot(a, ref[:, at], preferred_element_type=jnp.float32)
            total = part if total is None else total + part
        out_ref[:, at] = total.astype(out_ref.dtype)


def mix(own, where, back, weights):
    return call(
        functools.partial(mix_kernel, own), 2 * 256 * 1024 * 2048,
        out_shape=jax.ShapeDtypeStruct((256, 2048), jnp.float32 if own else jnp.bfloat16),
        in_specs=[SMEM] + [VMEM] * 5, out_specs=VMEM,
    )(where, back, *weights)


def after(value, *others):
    return lax.optimization_barrier((value, *others))[0]


def layer(hidden, gate, wq, wk, wv, wo):
    x = lax.axis_index("x")
    c = lax.axis_index("core")
    first = c == 0
    where = jnp.stack([x, c, lax.axis_index("yl")]).astype(jnp.int32)
    own = hidden.reshape(256, 2048)
    homes = ("z", "yh", "yl")

    beside = swap(own, "yl")
    shard = jnp.concatenate([jnp.where(first, wk, wv), swap(jnp.where(first, wv, wk))], axis=0)
    kv_weights = gather_x(shard)
    keep, give = arrange(where, wq)
    shard = jnp.concatenate([keep, swap(give)], axis=0)
    q_weights = fetch_x(after(shard, kv_weights[1], kv_weights[2]))
    other = swap(own)

    by_unit = jnp.transpose(gate.reshape(2, POS, 2, 4, 2, 2), (4, 0, 3, 2, 5, 1))
    mine = jnp.where(first, by_unit[0], by_unit[1])
    got = swap(jnp.where(first, by_unit[1], by_unit[0]))
    gates = jnp.where(first, jnp.stack([mine, got]), jnp.stack([got, mine]))
    gates = gates.reshape(BLOCKS, 2, POS)

    kv = project_kv(where, (own, other), gates, kv_weights)
    kv = exchange(kv, homes)
    tokens = (own, other, beside, swap(beside))
    query = project_q(where, tokens, q_weights)
    theirs = swap(kv[:, :64])
    query = exchange(query, ("z", "yh"))

    halves = wo.reshape(2, 128, 2048)
    mine = jnp.where(first, halves[0], halves[1])
    got = swap(jnp.where(first, halves[1], halves[0]))
    shard = jnp.where(first, jnp.concatenate([mine, got]), jnp.concatenate([got, mine]))
    o_weights = fetch_x(after(shard, *q_weights[1:]))

    back = exchange(attend(where, query, kv, theirs), homes)
    theirs = swap(mix(False, where, back, o_weights))
    mine = mix(True, where, back, o_weights)
    mixed = mine + theirs.astype(jnp.float32)
    return mixed.astype(jnp.bfloat16).reshape(2, POS, 2048)


def solution(mesh):
    fine = Mesh(mesh.devices.reshape(Z, 2, 2, X, 2), ("z", "yh", "yl", "x", "core"))
    dp, sp = ("x", "core"), ("z", "yh", "yl")
    placed = (P(dp, sp, None), P(dp, sp, None), P(dp, None), P(dp, None), P(dp, None), P(dp, None))
    return jax.shard_map(
        layer, mesh=fine, in_specs=placed, out_specs=P(dp, sp, None), check_vma=False
    )
```
